32 devices in a mesh: rep: 2 (over x), fs: 8 (over z, y), tp: 2 (over core).
Axes of the slice: x: 2, y: 2, z: 4, core: 2. Of those that a mesh axis runs over, the one named last changes fastest.
Arguments:
- tokens: bfloat16 [8192, 2048], P(('rep', 'fs')), may hold values from -3 to 3
- mixer_gain: float32 [2048], replicated, may hold values from 0.1 to 1.9
- mix_weight: bfloat16 [2048, 1024], P('fs', 'tp'), may hold values from -0.125 to 0.125
- mixer_conv: float32 [4, 1024], P(None, 'tp'), may hold values from -3 to 3
- mixer_offset: float32 [1024], P('tp'), may hold values from -0.06 to 0.06
- recur_weight: bfloat16 [8, 128, 128], P('tp'), may hold values from -0.5 to 0.5
- recur_bias: float32 [1024], P('tp'), may hold values from -3 to 3
- input_weight: bfloat16 [8, 128, 128], P('tp'), may hold values from -0.5 to 0.5
- input_bias: float32 [1024], P('tp'), may hold values from 1 to 3
- decay_logit: float32 [1024], P('tp'), may hold values from 4 to 11
- out_weight: bfloat16 [1024, 2048], P('tp', 'fs'), may hold values from -0.375 to 0.375
- channel_gain: float32 [2048], replicated, may hold values from 0.1 to 1.9
- gate_weight: bfloat16 [2048, 6144], P('fs', 'tp'), may hold values from -0.125 to 0.125
- up_weight: bfloat16 [2048, 6144], P('fs', 'tp'), may hold values from -0.125 to 0.125
- gate_conv: float32 [3, 6144], P(None, 'tp'), may hold values from -3.5 to 3.5
- gate_offset: float32 [6144], P('tp'), may hold values from -3 to 3
- down_weight: bfloat16 [6144, 2048], P('tp', 'fs'), may hold values from -0.078125 to 0.078125
Outputs:
- layer_out: bfloat16 [8192, 2048], P(('rep', 'fs'))
The draws below stay inside these ranges and needn't reach their ends.
All inputs are finite; a program needn't handle non-finite values.
Results may differ from the reference program's by a relative error of at most 0.023.
Values may be sent and summed in bfloat16 or wider, within the bound.
A program may use at most 128 MiB of HBM per device.

```python
import jax
import jax.numpy as jnp
from jax import lax

D = 2048
LRU = 1024
BLOCKS = 8
BLOCK_DIM = 128
MIX_TAPS = 4
FF = 6144
MLP_TAPS = 3
SEQLEN = 512
SEQS = 16
TOKENS = 8192
N_TP = 2


def draw_decay_logit(key, part):
    pick_key = jax.random.fold_in(key, 11)
    slow_key = jax.random.fold_in(key, 12)
    fast_key = jax.random.fold_in(key, 13)
    fast_share = 0.5
    fast = jax.random.bernoulli(pick_key, fast_share, (LRU,))
    slow_rate = jax.random.uniform(slow_key, (LRU,), jnp.float32, 1.0, 2.3) / SEQLEN
    fast_rate = jax.random.uniform(fast_key, (LRU,), jnp.float32, 0.02, 0.08)
    rate = jnp.where(fast, fast_rate, slow_rate) / 8.0
    return -rate - jnp.log(-jnp.expm1(-rate))


def steps_of(rng, shape, pieces, least, top_value):
    loudness, own = 1.0, jax.random.fold_in(rng, 6)
    for axis_at, blocks in pieces:
        draws = jnp.exp(jax.random.uniform(jax.random.fold_in(own, axis_at), (blocks,), jnp.float32, least / len(pieces), top_value / len(pieces)))
        loudness = loudness * jnp.repeat(draws, shape[axis_at] // blocks).reshape([-1 if axis == axis_at else 1 for axis in range(len(shape))])
    return loudness


def scatter_about(own_key, shape, spread, bound, cuts=(), kind=jnp.bfloat16):
    entries = spread * jax.random.normal(own_key, shape, jnp.float32)
    if cuts:
        entries = entries * steps_of(own_key, shape, cuts, -0.22, 0.18)
    return jnp.clip(entries, -bound, bound).astype(kind)


def setup_inputs(seed: int = 0) -> dict:
    keys = jax.random.split(jax.random.key(seed), 18)
    return {
        "tokens": scatter_about(keys[0], (TOKENS, D), 0.5, 3.0, ((0, 16),)),
        "mixer_gain": jnp.clip(1.0 + 0.18 * jax.random.normal(keys[1], (D,), jnp.float32), 0.1, 1.9),
        "mix_weight": scatter_about(keys[2], (D, LRU), D ** -0.5, 0.125, ((0, 8), (1, 2))),
        "mixer_conv": scatter_about(keys[3], (MIX_TAPS, LRU), MIX_TAPS ** -0.5, 3.0, ((1, 2),), jnp.float32),
        "mixer_offset": scatter_about(keys[4], (LRU,), 0.02, 0.06, ((0, 2),), jnp.float32),
        "recur_weight": scatter_about(keys[5], (BLOCKS, BLOCK_DIM, BLOCK_DIM), BLOCK_DIM ** -0.5, 0.5, ((0, 2),)),
        "recur_bias": scatter_about(keys[6], (LRU,), 0.5, 3.0, ((0, 2),), jnp.float32),
        "input_weight": scatter_about(keys[7], (BLOCKS, BLOCK_DIM, BLOCK_DIM), BLOCK_DIM ** -0.5, 0.5, ((0, 2),)),
        "input_bias": jnp.clip(1.0 + 2.0 * jax.random.uniform(keys[8], (LRU,), jnp.float32) ** steps_of(keys[8], (LRU,), ((0, 2),), -0.2, 0.2), 1.0, 3.0),
        "decay_logit": draw_decay_logit(jax.random.fold_in(keys[17], 71), 0),
        "out_weight": scatter_about(keys[10], (LRU, D), (LRU // 4) ** -0.5, 0.375, ((0, 2), (1, 8))),
        "channel_gain": jnp.clip(1.0 + 0.18 * jax.random.normal(keys[11], (D,), jnp.float32), 0.1, 1.9),
        "gate_weight": scatter_about(keys[12], (D, FF), D ** -0.5, 0.125, ((0, 8), (1, 2))),
        "up_weight": scatter_about(keys[13], (D, FF), D ** -0.5, 0.125, ((0, 8), (1, 2))),
        "gate_conv": scatter_about(keys[14], (MLP_TAPS, FF), MLP_TAPS ** -0.5, 3.5, ((1, 2),), jnp.float32),
        "gate_offset": scatter_about(keys[15], (FF,), 0.5, 3.0, ((0, 2),), jnp.float32),
        "down_weight": scatter_about(keys[16], (FF, D), FF ** -0.5, 0.078125, ((0, 2), (1, 8))),
    }


epsilon = 1e-06
lru_scale = 8.0

def rms_rows(values, gain_row):
    widened = values.astype(jnp.float32)
    scaled = widened * lax.rsqrt(lax.optimization_barrier(jnp.mean(widened * widened, axis=-1, keepdims=True)) + epsilon)
    return (scaled * gain_row).astype(jnp.bfloat16)

def causal_conv(values, tap_rows, offset):
    width = tap_rows.shape[0]
    length = values.shape[-2]
    padding = [(0, 0)] * (values.ndim - 2) + [(width - 1, 0), (0, 0)]
    padded = jnp.pad(values, padding)
    total = offset + padded[..., 0:length, :] * tap_rows[0]
    for tap_index in range(1, width):
        total = total + padded[..., tap_index:tap_index + length, :] * tap_rows[tap_index]
    return total

def linear_combine(earlier, latter):
    decay_early, sum_early = earlier
    decay_late, sum_late = latter
    return (decay_early * decay_late, decay_late * sum_early + sum_late)

def lru_recur(recur_gate, input_gate, smoothed, decay_logit, axis):
    log_decay = lru_scale * recur_gate * jax.nn.log_sigmoid(decay_logit)
    drive = jnp.sqrt(-jnp.expm1(2.0 * log_decay)) * (input_gate * smoothed.astype(jnp.float32))
    _, states = lax.associative_scan(linear_combine, (jnp.exp(log_decay), drive), axis=axis)
    return states.astype(jnp.bfloat16)

def group_sums(left, right, groups):
    width = left.shape[1] // groups

    def add_group(total, index):
        left_part = lax.dynamic_slice_in_dim(left, index * width, width, 1)
        right_part = lax.dynamic_slice_in_dim(right, index * width, width, 0)
        partial_sum = jnp.dot(left_part, right_part, preferred_element_type=jnp.float32)
        rounded = lax.optimization_barrier(partial_sum.astype(jnp.bfloat16))
        return (total + rounded.astype(jnp.float32), None)
    start_total = jnp.zeros((left.shape[0], right.shape[1]), jnp.float32)
    total, _ = lax.scan(add_group, start_total, jnp.arange(groups, dtype=jnp.int32))
    return total

def block_gate(blocked, weight, bias):
    product = jnp.einsum('slhi,hij->slhj', blocked, weight.astype(jnp.float32))
    return jax.nn.sigmoid(product.reshape(SEQS, SEQLEN, LRU) + bias)

def reference(tokens, mixer_gain, mix_weight, mixer_conv, mixer_offset, recur_weight, recur_bias, input_weight, input_bias, decay_logit, out_weight, channel_gain, gate_weight, up_weight, gate_conv, gate_offset, down_weight):
    normed = rms_rows(tokens, mixer_gain)
    branch = jnp.dot(normed, mix_weight, preferred_element_type=jnp.float32).astype(jnp.bfloat16)
    branch = branch.reshape(SEQS, SEQLEN, LRU)
    smoothed = causal_conv(branch.astype(jnp.float32), mixer_conv, mixer_offset).astype(jnp.bfloat16)
    blocked = smoothed.reshape(SEQS, SEQLEN, BLOCKS, BLOCK_DIM).astype(jnp.float32)
    recur_gate = block_gate(blocked, recur_weight, recur_bias)
    input_gate = block_gate(blocked, input_weight, input_bias)
    recurrent = lru_recur(recur_gate, input_gate, smoothed, decay_logit, 1).reshape(TOKENS, LRU)
    mixer_sum = group_sums(recurrent, out_weight, N_TP)
    residual = (tokens.astype(jnp.float32) + mixer_sum).astype(jnp.bfloat16)
    normed_mlp = rms_rows(residual, channel_gain)
    gate_rows = jnp.dot(normed_mlp, gate_weight, preferred_element_type=jnp.float32).astype(jnp.bfloat16)
    up_rows = jnp.dot(normed_mlp, up_weight, preferred_element_type=jnp.float32).astype(jnp.bfloat16)
    gate_mixed = causal_conv(gate_rows.reshape(SEQS, SEQLEN, FF).astype(jnp.float32), gate_conv, gate_offset)
    hidden = jax.nn.gelu(gate_mixed) * up_rows.reshape(SEQS, SEQLEN, FF).astype(jnp.float32)
    hidden = hidden.astype(jnp.bfloat16).reshape(TOKENS, FF)
    mlp_sum = group_sums(hidden, down_weight, N_TP)
    return (residual.astype(jnp.float32) + mlp_sum).astype(jnp.bfloat16)
```

```python
import functools

import jax
import jax.numpy as jnp
from jax import lax
from jax.experimental import pallas as pl
from jax.experimental.pallas import tpu as pltpu
from jax.sharding import PartitionSpec as P

epsilon = 1e-06
lru_scale = 8.0


def rms_rows(values, gain_row):
    widened = values.astype(jnp.float32)
    scaled = widened * lax.rsqrt(jnp.mean(widened * widened, axis=-1, keepdims=True) + epsilon)
    return (scaled * gain_row).astype(jnp.bfloat16)


def causal_conv(values, tap_rows, offset):
    width = tap_rows.shape[0]
    length = values.shape[-2]
    padding = [(0, 0)] * (values.ndim - 2) + [(width - 1, 0), (0, 0)]
    padded = jnp.pad(values, padding)
    total = offset + padded[..., 0:length, :] * tap_rows[0]
    for tap_index in range(1, width):
        total = total + padded[..., tap_index : tap_index + length, :] * tap_rows[tap_index]
    return total


def one_minus_exp(v):
    series = 1.0 + v * (1.0 / 7.0)
    for order in (6.0, 5.0, 4.0, 3.0, 2.0):
        series = 1.0 + v * (1.0 / order) * series
    return jnp.where(v > -0.25, -v * series, 1.0 - jnp.exp(v))


def mixer_kernel(
    branch_ref, taps_ref, offset_ref, recur_ref, recur_bias_ref, input_ref, input_bias_ref, rate_ref, out_ref
):
    branch = branch_ref[...].astype(jnp.float32)
    length = branch.shape[0]
    width = taps_ref.shape[0]
    rows = lax.broadcasted_iota(jnp.int32, branch.shape, 0)

    def shifted(values, step, fill):
        return jnp.where(rows >= step, pltpu.roll(values, step, 0), fill)

    total = offset_ref[...] + branch * taps_ref[width - 1 : width, :]
    for back in range(1, width):
        total = total + shifted(branch, back, 0.0) * taps_ref[width - 1 - back : width - back, :]
    smoothed = total.astype(jnp.bfloat16)
    recur = jnp.dot(smoothed, recur_ref[0], preferred_element_type=jnp.float32)
    recur_gate = jax.nn.sigmoid(recur + recur_bias_ref[...])
    gated = jnp.dot(smoothed, input_ref[0], preferred_element_type=jnp.float32)
    input_gate = jax.nn.sigmoid(gated + input_bias_ref[...])
    log_decay = recur_gate * rate_ref[...]
    state = jnp.sqrt(one_minus_exp(2.0 * log_decay)) * (input_gate * smoothed.astype(jnp.float32))
    decay = jnp.exp(log_decay)
    step = 1
    while step < length:
        state = state + decay * shifted(state, step, 0.0)
        if 2 * step < length:
            decay = decay * shifted(decay, step, 1.0)
        step *= 2
    out_ref[...] = state.astype(jnp.bfloat16)


def mixer(branch, taps, offset, recur_weight, recur_bias, input_weight, input_bias, rate):
    length, channels = branch.shape
    blocks, dim, _ = recur_weight.shape
    column = lambda rows: pl.BlockSpec((rows, dim), lambda k: (0, k))
    square = pl.BlockSpec((1, dim, dim), lambda k: (k, 0, 0))
    row = lambda v: v.reshape(1, channels)
    return pl.pallas_call(
        mixer_kernel,
        name="mixer",
        grid=(blocks,),
        in_specs=[
            column(length),
            column(taps.shape[0]),
            column(1),
            square,
            column(1),
            square,
            column(1),
            column(1),
        ],
        out_specs=column(length),
        out_shape=jax.ShapeDtypeStruct((length, channels), jnp.bfloat16),
        cost_estimate=pl.CostEstimate(
            flops=60 * length * channels + 4 * length * channels * dim,
            bytes_accessed=4 * length * channels,
            transcendentals=5 * length * channels,
        ),
    )(
        branch,
        taps,
        row(offset),
        recur_weight,
        row(recur_bias),
        input_weight,
        row(input_bias),
        row(rate),
    )


def shift(values, axis, count, step):
    return lax.ppermute(values, axis, [(i, (i + step) % count) for i in range(count)])


def take(values, index, size, axis=0):
    return lax.dynamic_slice_in_dim(values, index * size, size, axis)


def scatter_rows(partial, n_tp, me):
    size = partial.shape[0] // n_tp
    total = take(partial, me, size).astype(jnp.float32)
    for step in range(1, n_tp):
        sent = take(partial, lax.rem(me + step, n_tp), size)
        total = total + shift(sent, "tp", n_tp, step).astype(jnp.float32)
    return total


def collect_rows(share, n_tp, me):
    size = share.shape[0]
    if n_tp == 2:
        other = shift(share, "tp", n_tp, 1)
        first = jnp.where(me == 0, share, other)
        second = jnp.where(me == 0, other, share)
        return jnp.concatenate([first, second], axis=0)
    whole = jnp.zeros((size * n_tp, share.shape[1]), share.dtype)
    whole = lax.dynamic_update_slice_in_dim(whole, share, me * size, 0)
    for step in range(1, n_tp):
        got = shift(share, "tp", n_tp, step)
        whole = lax.dynamic_update_slice_in_dim(whole, got, lax.rem(me - step + n_tp, n_tp) * size, 0)
    return whole


def local(
    n_rep,
    n_tp,
    tokens,
    mixer_gain,
    mix_weight,
    mixer_conv,
    mixer_offset,
    recur_weight,
    recur_bias,
    input_weight,
    input_bias,
    decay_logit,
    out_weight,
    channel_gain,
    gate_weight,
    up_weight,
    gate_conv,
    gate_offset,
    down_weight,
):
    rep = lax.axis_index("rep")
    tp = lax.axis_index("tp")
    length = tokens.shape[0]
    units = gate_weight.shape[1] // n_rep

    mixer_full = lax.all_gather(mix_weight, "fs", axis=0, tiled=True)
    out_full = lax.all_gather(out_weight, "fs", axis=1, tiled=True)
    gate_full = lax.all_gather(take(gate_weight, rep, units, 1), "fs", axis=0, tiled=True)
    up_full = lax.all_gather(take(up_weight, rep, units, 1), "fs", axis=0, tiled=True)
    down_full = lax.all_gather(take(down_weight, rep, units, 0), "fs", axis=1, tiled=True)
    gate_taps = take(gate_conv, rep, units, 1)
    gate_base = take(gate_offset, rep, units, 0)

    normed = rms_rows(tokens, mixer_gain)
    branch = jnp.dot(normed, mixer_full, preferred_element_type=jnp.float32).astype(jnp.bfloat16)
    recurrent = mixer(
        branch,
        mixer_conv,
        mixer_offset,
        recur_weight,
        recur_bias,
        input_weight,
        input_bias,
        lru_scale * jax.nn.log_sigmoid(decay_logit),
    )
    mixer_term = jnp.dot(recurrent, out_full, preferred_element_type=jnp.float32)
    mixer_share = scatter_rows(mixer_term.astype(jnp.bfloat16), n_tp, tp)
    rows = length // n_tp
    residual = (take(tokens, tp, rows).astype(jnp.float32) + mixer_share).astype(jnp.bfloat16)
    normed_share = rms_rows(residual, channel_gain)

    shares = [normed_share]
    for step in range(1, n_rep):
        shares.append(shift(normed_share, "rep", n_rep, step))

    def channel_mixer(share):
        rows_in = collect_rows(share, n_tp, tp)
        gate_rows = jnp.dot(rows_in, gate_full, preferred_element_type=jnp.float32)
        up_rows = jnp.dot(rows_in, up_full, preferred_element_type=jnp.float32)
        gate_rows = gate_rows.astype(jnp.bfloat16)
        up_rows = up_rows.astype(jnp.bfloat16)
        gate_mixed = causal_conv(gate_rows.astype(jnp.float32), gate_taps, gate_base)
        hidden = (jax.nn.gelu(gate_mixed) * up_rows.astype(jnp.float32)).astype(jnp.bfloat16)
        return jnp.dot(hidden, down_full, preferred_element_type=jnp.float32).astype(jnp.bfloat16)

    own_terms = channel_mixer(shares[0])
    total = None
    for step in range(1, n_rep):
        summed = scatter_rows(channel_mixer(shares[step]), n_tp, tp).astype(jnp.bfloat16)
        back = shift(summed, "rep", n_rep, -step).astype(jnp.float32)
        total = back if total is None else total + back
    own = scatter_rows(own_terms, n_tp, tp)
    total = own if total is None else own + total
    result = (residual.astype(jnp.float32) + total).astype(jnp.bfloat16)
    return collect_rows(result, n_tp, tp)


def solution(mesh):
    in_specs = (
        P(("rep", "fs"), None),
        P(),
        P("fs", "tp"),
        P(None, "tp"),
        P("tp"),
        P("tp", None, None),
        P("tp"),
        P("tp", None, None),
        P("tp"),
        P("tp"),
        P("tp", "fs"),
        P(),
        P("fs", "tp"),
        P("fs", "tp"),
        P(None, "tp"),
        P("tp"),
        P("tp", "fs"),
    )
    out_specs = P(("rep", "fs"), None)
    body = functools.partial(local, mesh.shape["rep"], mesh.shape["tp"])
    return jax.shard_map(body, mesh=mesh, in_specs=in_specs, out_specs=out_specs, check_vma=False)
```

```python
import functools

import jax
import jax.numpy as jnp
from jax import lax
from jax.experimental import pallas as pl
from jax.experimental.pallas import tpu as pltpu
from jax.sharding import PartitionSpec as P

epsilon = 1e-06
lru_scale = 8.0


def rms_rows(values, gain_row):
    widened = values.astype(jnp.float32)
    scaled = widened * lax.rsqrt(jnp.mean(widened * widened, axis=-1, keepdims=True) + epsilon)
    return (scaled * gain_row).astype(jnp.bfloat16)


def causal_conv(values, tap_rows, offset):
    width = tap_rows.shape[0]
    length = values.shape[-2]
    padding = [(0, 0)] * (values.ndim - 2) + [(width - 1, 0), (0, 0)]
    padded = jnp.pad(values, padding)
    total = offset + padded[..., 0:length, :] * tap_rows[0]
    for tap_index in range(1, width):
        total = total + padded[..., tap_index : tap_index + length, :] * tap_rows[tap_index]
    return total


def one_minus_exp(v):
    series = 1.0 + v * (1.0 / 7.0)
    for order in (6.0, 5.0, 4.0, 3.0, 2.0):
        series = 1.0 + v * (1.0 / order) * series
    return jnp.where(v > -0.25, -v * series, 1.0 - jnp.exp(v))


def mixer_kernel(
    branch_ref, taps_ref, offset_ref, recur_ref, recur_bias_ref, input_ref, input_bias_ref, rate_ref, out_ref
):
    branch = branch_ref[...].astype(jnp.float32)
    length = branch.shape[0]
    width = taps_ref.shape[0]
    rows = lax.broadcasted_iota(jnp.int32, branch.shape, 0)

    def shifted(values, step, fill):
        return jnp.where(rows >= step, pltpu.roll(values, step, 0), fill)

    total = offset_ref[...] + branch * taps_ref[width - 1 : width, :]
    for back in range(1, width):
        total = total + shifted(branch, back, 0.0) * taps_ref[width - 1 - back : width - back, :]
    smoothed = total.astype(jnp.bfloat16)
    recur = jnp.dot(smoothed, recur_ref[0], preferred_element_type=jnp.float32)
    recur_gate = jax.nn.sigmoid(recur + recur_bias_ref[...])
    gated = jnp.dot(smoothed, input_ref[0], preferred_element_type=jnp.float32)
    input_gate = jax.nn.sigmoid(gated + input_bias_ref[...])
    log_decay = recur_gate * rate_ref[...]
    state = jnp.sqrt(one_minus_exp(2.0 * log_decay)) * (input_gate * smoothed.astype(jnp.float32))
    decay = jnp.exp(log_decay)
    step = 1
    while step < length:
        state = state + decay * shifted(state, step, 0.0)
        if 2 * step < length:
            decay = decay * shifted(decay, step, 1.0)
        step *= 2
    out_ref[...] = state.astype(jnp.bfloat16)


def mixer(branch, taps, offset, recur_weight, recur_bias, input_weight, input_bias, rate):
    length, channels = branch.shape
    blocks, dim, _ = recur_weight.shape
    column = lambda rows: pl.BlockSpec((rows, dim), lambda k: (0, k))
    square = pl.BlockSpec((1, dim, dim), lambda k: (k, 0, 0))
    row = lambda v: v.reshape(1, channels)
    return pl.pallas_call(
        mixer_kernel,
        name="mixer",
        grid=(blocks,),
        in_specs=[
            column(length),
            column(taps.shape[0]),
            column(1),
            square,
            column(1),
            square,
            column(1),
            column(1),
        ],
        out_specs=column(length),
        out_shape=jax.ShapeDtypeStruct((length, channels), jnp.bfloat16),
        cost_estimate=pl.CostEstimate(
            flops=60 * length * channels + 4 * length * channels * dim,
            bytes_accessed=4 * length * channels,
            transcendentals=5 * length * channels,
        ),
    )(
        branch,
        taps,
        row(offset),
        recur_weight,
        row(recur_bias),
        input_weight,
        row(input_bias),
        row(rate),
    )


def shift(values, axis, count, step):
    return lax.ppermute(values, axis, [(i, (i + step) % count) for i in range(count)])


def take(values, index, size, axis=0):
    return lax.dynamic_slice_in_dim(values, index * size, size, axis)


def pair_gather(weight, count, axis):
    groups = [list(range(parity, count, 2)) for parity in range(2)]
    own = lax.all_gather(weight, "fs", axis=axis, axis_index_groups=groups, tiled=True)
    other = lax.ppermute(own, "fs", [(i, i ^ 1) for i in range(count)])
    return own, other


def pair_columns(values, count, parity):
    rows, width = values.shape
    size = width // count
    blocks = [values[:, i * size : (i + 1) * size] for i in range(count)]
    even = jnp.concatenate(blocks[0::2], axis=1)
    odd = jnp.concatenate(blocks[1::2], axis=1)
    return jnp.where(parity == 0, even, odd), jnp.where(parity == 0, odd, even)


def scatter_rows(partial, n_tp, me):
    size = partial.shape[0] // n_tp
    total = take(partial, me, size).astype(jnp.float32)
    for step in range(1, n_tp):
        sent = take(partial, lax.rem(me + step, n_tp), size)
        total = total + shift(sent, "tp", n_tp, step).astype(jnp.float32)
    return total


def collect_rows(share, n_tp, me):
    size = share.shape[0]
    if n_tp == 2:
        other = shift(share, "tp", n_tp, 1)
        first = jnp.where(me == 0, share, other)
        second = jnp.where(me == 0, other, share)
        return jnp.concatenate([first, second], axis=0)
    whole = jnp.zeros((size * n_tp, share.shape[1]), share.dtype)
    whole = lax.dynamic_update_slice_in_dim(whole, share, me * size, 0)
    for step in range(1, n_tp):
        got = shift(share, "tp", n_tp, step)
        whole = lax.dynamic_update_slice_in_dim(whole, got, lax.rem(me - step + n_tp, n_tp) * size, 0)
    return whole


def local(
    n_rep,
    n_fs,
    n_tp,
    tokens,
    mixer_gain,
    mix_weight,
    mixer_conv,
    mixer_offset,
    recur_weight,
    recur_bias,
    input_weight,
    input_bias,
    decay_logit,
    out_weight,
    channel_gain,
    gate_weight,
    up_weight,
    gate_conv,
    gate_offset,
    down_weight,
):
    rep = lax.axis_index("rep")
    tp = lax.axis_index("tp")
    parity = lax.rem(lax.axis_index("fs"), 2)
    length = tokens.shape[0]
    units = gate_weight.shape[1] // n_rep

    both = jnp.concatenate([mix_weight, out_weight.T], axis=1)
    both_full = lax.all_gather(both, "fs", axis=0, tiled=True)
    channels = mix_weight.shape[1]
    mixer_full, out_full = both_full[:, :channels], both_full[:, channels:]
    gate_own, gate_other = pair_gather(take(gate_weight, rep, units, 1), n_fs, 0)
    up_own, up_other = pair_gather(take(up_weight, rep, units, 1), n_fs, 0)
    down_full = lax.all_gather(take(down_weight, rep, units, 0), "fs", axis=1, tiled=True)
    gate_taps = take(gate_conv, rep, units, 1)
    gate_base = take(gate_offset, rep, units, 0)

    normed = rms_rows(tokens, mixer_gain)
    branch = jnp.dot(normed, mixer_full, preferred_element_type=jnp.float32).astype(jnp.bfloat16)
    recurrent = mixer(
        branch,
        mixer_conv,
        mixer_offset,
        recur_weight,
        recur_bias,
        input_weight,
        input_bias,
        lru_scale * jax.nn.log_sigmoid(decay_logit),
    )
    mixer_term = lax.dot_general(
        recurrent, out_full, (((1,), (1,)), ((), ())), preferred_element_type=jnp.float32
    )
    mixer_share = scatter_rows(mixer_term.astype(jnp.bfloat16), n_tp, tp)
    rows = length // n_tp
    residual = (take(tokens, tp, rows).astype(jnp.float32) + mixer_share).astype(jnp.bfloat16)
    normed_share = rms_rows(residual, channel_gain)

    shares = [normed_share]
    for step in range(1, n_rep):
        shares.append(shift(normed_share, "rep", n_rep, step))

    def channel_mixer(share):
        rows_in = collect_rows(share, n_tp, tp)
        left, right = pair_columns(rows_in, n_fs, parity)
        gate_rows = jnp.dot(left, gate_own, preferred_element_type=jnp.float32)
        gate_rows = gate_rows + jnp.dot(right, gate_other, preferred_element_type=jnp.float32)
        up_rows = jnp.dot(left, up_own, preferred_element_type=jnp.float32)
        up_rows = up_rows + jnp.dot(right, up_other, preferred_element_type=jnp.float32)
        gate_rows = gate_rows.astype(jnp.bfloat16)
        up_rows = up_rows.astype(jnp.bfloat16)
        gate_mixed = causal_conv(gate_rows.astype(jnp.float32), gate_taps, gate_base)
        hidden = (jax.nn.gelu(gate_mixed) * up_rows.astype(jnp.float32)).astype(jnp.bfloat16)
        return jnp.dot(hidden, down_full, preferred_element_type=jnp.float32).astype(jnp.bfloat16)

    own_terms = channel_mixer(shares[0])
    total = None
    for step in range(1, n_rep):
        summed = scatter_rows(channel_mixer(shares[step]), n_tp, tp).astype(jnp.bfloat16)
        back = shift(summed, "rep", n_rep, -step).astype(jnp.float32)
        total = back if total is None else total + back
    own = scatter_rows(own_terms, n_tp, tp)
    total = own if total is None else own + total
    result = (residual.astype(jnp.float32) + total).astype(jnp.bfloat16)
    return collect_rows(result, n_tp, tp)


def solution(mesh):
    in_specs = (
        P(("rep", "fs"), None),
        P(),
        P("fs", "tp"),
        P(None, "tp"),
        P("tp"),
        P("tp", None, None),
        P("tp"),
        P("tp", None, None),
        P("tp"),
        P("tp"),
        P("tp", "fs"),
        P(),
        P("fs", "tp"),
        P("fs", "tp"),
        P(None, "tp"),
        P("tp"),
        P("tp", "fs"),
    )
    out_specs = P(("rep", "fs"), None)
    body = functools.partial(local, mesh.shape["rep"], mesh.shape["fs"], mesh.shape["tp"])
    return jax.shard_map(body, mesh=mesh, in_specs=in_specs, out_specs=out_specs, check_vma=False)
```
